32 devices in a mesh: ep: 4 (over y, x), tp: 8 (over z, core).
Axes of the slice: x: 2, y: 2, z: 4, core: 2. Of those that a mesh axis runs over, the one named last changes fastest.
Arguments:
- tokens: bfloat16 [1024, 1024], P(('ep', 'tp')), may hold values from -6 to 6
- norm_gain: float32 [1024], replicated, may hold values from 0.5 to 1.5
- routing: int32 [1024, 2], P('ep'), may hold values from 0 to 7, as said below
- gate_share: float32 [1024, 2], P('ep'), may hold values from 0.5 to 1.5
- w_gate: bfloat16 [8, 1024, 256], P('ep', None, 'tp'), may hold values from -0.1875 to 0.1875
- w_up: bfloat16 [8, 1024, 256], P('ep', None, 'tp'), may hold values from -0.1875 to 0.1875
- w_down: bfloat16 [8, 256, 1024], P('ep', 'tp'), may hold values from -0.375 to 0.375
Outputs:
- mixed_out: bfloat16 [1024, 1024], P('ep', 'tp')
The draws below stay inside these ranges and needn't reach their ends.
Inputs may be any that keep to these rules, and one draw needn't show every extreme that they name: `routing`: each row names two different experts whose ids lie in the same block of 2 consecutive ids. In each aligned block of 256 rows (the tokens of one index of ep) no expert is named by more than 128 rows, and some expert is named by exactly 128.
All inputs are finite; a program needn't handle non-finite values.
Results may differ from the reference program's by a relative error of at most 0.0015.
Values may be sent and summed in bfloat16 or wider, within the bound.
A program may use at most 64 MiB of HBM per device.

```python
import jax
import jax.numpy as jnp
from jax import lax

D = 1024
HIDDEN_SIZE = 256
TOPK = 2
GROUPS = 4
GROUP_TOK = 256
TOKENS = 1024
EXPERTS = 8
CAP = 128
N_EP = 4


def draw_routing(key, part):
    block_count = TOKENS // GROUP_TOK
    group_size = EXPERTS // GROUPS
    eighth = GROUP_TOK // 8
    position = jnp.arange(GROUP_TOK, dtype=jnp.int32)
    group_slot = (position >= 4 * eighth).astype(jnp.int32) + (position >= 6 * eighth).astype(jnp.int32) + (position >= 7 * eighth).astype(jnp.int32)
    group_start = jnp.array([0, 4 * eighth, 6 * eighth, 7 * eighth], dtype=jnp.int32)[group_slot]
    within = position - group_start
    first_pick = within % group_size
    second = (within + 1) % group_size

    def inner_draw(sub_key):
        return jax.random.permutation(sub_key, group_size).astype(jnp.int32)

    def draw_block(block_key):
        key_order, key_group, key_inner, key_flip = jax.random.split(block_key, 4)
        token_order = jax.random.permutation(key_order, GROUP_TOK).astype(jnp.int32)
        group_label = jax.random.permutation(key_group, GROUPS).astype(jnp.int32)
        inner_order = jax.vmap(inner_draw)(jax.random.split(key_inner, GROUPS))
        label = group_label[group_slot]
        one_id = label * group_size + inner_order[label, first_pick]
        two_id = label * group_size + inner_order[label, second]
        flipped = jax.random.randint(key_flip, (GROUP_TOK,), 0, 2)
        left = jnp.where(flipped == 1, two_id, one_id)
        right = jnp.where(flipped == 1, one_id, two_id)
        paired = jnp.stack([left, right], axis=1)
        return paired[token_order].astype(jnp.int32)
    block_keys = jax.random.split(jax.random.fold_in(key, 11), block_count)
    return jax.vmap(draw_block)(block_keys).reshape(TOKENS, 2).astype(jnp.int32)


def level_of(stream_key, shape, shards, low, high):
    def one(dim, parts):
        draws = jax.random.uniform(jax.random.fold_in(jax.random.fold_in(stream_key, 6), dim), (parts,), jnp.float32, low / len(shards), high / len(shards))
        return jnp.repeat(jnp.exp(draws), shape[dim] // parts).reshape((-1,) + (1,) * (len(shape) - dim - 1))

    gain = one(*shards[0])
    for cut in shards[1:]:
        gain = gain * one(*cut)
    return gain


def gaussian(stream_key, dims, spread, bound, pieces=(), kind=jnp.bfloat16):
    entries = jax.random.normal(stream_key, dims, jnp.float32) * spread
    if len(pieces) > 0:
        entries = level_of(stream_key, dims, pieces, -0.22, 0.18) * entries
    return jnp.clip(entries, min=-bound, max=bound).astype(kind)


def setup_inputs(seed: int = 0) -> dict:
    seeds = jax.random.split(jax.random.key(seed), 8)
    tokens = gaussian(seeds[0], (TOKENS, D), 1.0, 6.0, ((0, 32),))
    norm_gain = jnp.clip(1.0 + 0.1 * jax.random.normal(seeds[1], (D,), jnp.float32), 0.5, 1.5)
    routing = draw_routing(jax.random.fold_in(seeds[7], 71), 0)
    gate_share = jnp.clip(0.5 + 1.0 * jax.random.uniform(seeds[3], (TOKENS, TOPK), jnp.float32) ** level_of(seeds[3], (TOKENS, TOPK), ((0, 4),), -0.2, 0.2), 0.5, 1.5)
    w_gate = gaussian(seeds[4], (EXPERTS, D, HIDDEN_SIZE), D ** -0.5, 0.1875, ((0, 4), (2, 8)))
    w_up = gaussian(seeds[5], (EXPERTS, D, HIDDEN_SIZE), D ** -0.5, 0.1875, ((0, 4), (2, 8)))
    w_down = gaussian(seeds[6], (EXPERTS, HIDDEN_SIZE, D), HIDDEN_SIZE ** -0.5, 0.375, ((0, 4), (1, 8)))
    return {"tokens": tokens, "norm_gain": norm_gain, "routing": routing, "gate_share": gate_share, "w_gate": w_gate, "w_up": w_up, "w_down": w_down}


epsilon = 1e-06

def norm_rows(tokens, norm_gain):
    as_float = tokens.astype(jnp.float32)
    scaled = as_float * lax.rsqrt(lax.optimization_barrier(jnp.mean(as_float * as_float, axis=-1, keepdims=True)) + epsilon)
    return (scaled * norm_gain.astype(jnp.float32)).astype(jnp.bfloat16)

def reference(tokens, norm_gain, routing, gate_share, w_gate, w_up, w_down):
    normed = norm_rows(tokens, norm_gain)
    experts = w_gate.shape[0]
    room_size = N_EP * CAP
    onehot = (routing[:, :, None] == jnp.arange(experts, dtype=jnp.int32)[None, None, :]).astype(jnp.int32)
    naming = lax.optimization_barrier(jnp.sum(onehot, axis=1)).astype(jnp.int32)
    ranking = (jnp.cumsum(naming, axis=0) - 1).astype(jnp.int32)

    def run_expert(expert):
        row_ids = jnp.nonzero(naming[:, expert] > 0, size=room_size, fill_value=0)[0].astype(jnp.int32)
        picked = normed[row_ids]
        gate_sum = jnp.dot(picked, w_gate[expert], preferred_element_type=jnp.float32)
        up_sum = jnp.dot(picked, w_up[expert], preferred_element_type=jnp.float32)
        hidden = (jax.nn.silu(gate_sum) * up_sum).astype(jnp.bfloat16)
        return jnp.dot(hidden, w_down[expert], preferred_element_type=jnp.float32).astype(jnp.bfloat16)
    outputs = lax.map(run_expert, jnp.arange(experts, dtype=jnp.int32))
    position = jnp.take_along_axis(ranking, routing, axis=1).astype(jnp.int32)
    picked_out = outputs[routing, position]
    mixed_out = lax.optimization_barrier(jnp.sum(gate_share[:, :, None] * picked_out.astype(jnp.float32), axis=1))
    return mixed_out.astype(jnp.bfloat16)
```

```python
import functools

import jax
import jax.numpy as jnp
from jax import lax
from jax.experimental import pallas as pl
from jax.experimental.pallas import tpu as pltpu
from jax.sharding import PartitionSpec as P

epsilon = 1e-06
MESH = pl.DeviceIdType.MESH
CHUNKS = 2


def kernel(ep_size, tp_size, cap, tok, gain, routing, share, wg, wu, wd, out,
           G, OH, OHT, XS, X, H, RS, RET, WC, WDR, BW,
           s1s, s1r, f1s, f1r, wds, wdr, x2s, x2r, xfs, xfr,
           h3s, h3r, hfs, hfr, r4s, r4r):
    g = lax.axis_index("ep")
    j = lax.axis_index("tp")
    Z = tp_size // 2
    z = j // 2
    core = j % 2
    partner = z * 2 + (1 - core)
    rows, D = tok.shape
    W = D // CHUNKS
    R2 = cap // 2
    hs = wg.shape[2]
    side = ep_size // 2

    def zpeer(k):
        return ((z + k) % Z) * 2 + core

    def zfrom(k):
        return (z + Z - k) % Z

    def epeer(d):
        return ((g // side + d // side) % side) * side + (g % side + d % side) % side

    def rc(src, dst, ss, rs, dev):
        return pltpu.make_async_remote_copy(src_ref=src, dst_ref=dst, send_sem=ss,
                                            recv_sem=rs, device_id=dev, device_id_type=MESH)

    sends = []

    def start(cp):
        cp.start()
        sends.append(cp)

    bar = pltpu.get_barrier_semaphore()
    for k in range(1, tp_size):
        pl.semaphore_signal(bar, inc=1, device_id=(g, (j + k) % tp_size), device_id_type=MESH)
    for d in range(1, ep_size):
        pl.semaphore_signal(bar, inc=1, device_id=(epeer(d), j), device_id_type=MESH)

    x = tok[...].astype(jnp.float32)
    normed = x * lax.rsqrt(jnp.mean(x * x, axis=-1, keepdims=True) + epsilon)
    normed = (normed * gain[...]).astype(jnp.bfloat16)

    def gblock(c, t):
        return G.at[c, pl.ds(pl.multiple_of(t * rows, rows), rows), :]

    for c in range(CHUNKS):
        G[c, pl.ds(pl.multiple_of(j * rows, rows), rows), :] = normed[:, c * W:(c + 1) * W]

    pl.semaphore_wait(bar, tp_size - 1 + ep_size - 1)

    zorder = [Z // 2] + [k for k in range(1, Z) if k != Z // 2]
    for c in range(CHUNKS):
        for k in zorder:
            start(rc(gblock(c, j), gblock(c, j), s1s.at[c, k], s1r.at[c, k], (g, zpeer(k))))
        start(rc(gblock(c, j), gblock(c, j), s1s.at[c, 0], s1r.at[c, 0], (g, partner)))
    cols = D // tp_size
    for k in range(1, tp_size):
        dst = (j + k) % tp_size
        start(rc(wd.at[:, :, pl.ds(pl.multiple_of(dst * cols, cols), cols)], WDR.at[j],
                 wds.at[k], wdr.at[k], (g, dst)))
    WDR[j] = wd[:, :, pl.ds(pl.multiple_of(j * cols, cols), cols)]

    n = routing.shape[0]
    local = wg.shape[0]
    rel = jnp.bitwise_xor(lax.div(routing[:, 0:1], jnp.int32(local)), g)
    hot = (lax.broadcasted_iota(jnp.int32, (n, 128), 1) == rel)
    low = lax.broadcasted_iota(jnp.int32, (n, n), 1) < lax.broadcasted_iota(jnp.int32, (n, n), 0)
    rank = jnp.dot(low.astype(jnp.bfloat16), hot.astype(jnp.bfloat16),
                   preferred_element_type=jnp.float32)
    pos = jnp.sum(jnp.where(hot, rank, 0.0), axis=1, keepdims=True)
    slot = rel.astype(jnp.float32) * cap + pos
    slots = ep_size * cap
    OHT[...] = (lax.broadcasted_iota(jnp.int32, (n, slots), 1).astype(jnp.float32)
                == slot).astype(jnp.bfloat16)
    slot_row = jnp.transpose(jnp.broadcast_to(slot, (n, 128)))[0:1, :]
    OH[...] = (lax.broadcasted_iota(jnp.int32, (slots, n), 0).astype(jnp.float32)
               == slot_row).astype(jnp.bfloat16)
    for e in range(2):
        WC[:, e * hs:(e + 1) * hs] = wg[e]
        WC[:, (2 + e) * hs:(3 + e) * hs] = wu[e]
    BW[...] = jnp.zeros_like(BW)

    half = pl.multiple_of(core * R2, R2)
    other = pl.multiple_of((1 - core) * R2, R2)
    eorder = [ep_size - 1] + list(range(1, ep_size - 1))

    for c in range(CHUNKS):
        for k in [0] + list(range(1, Z)):
            if k == 0:
                src = gblock(c, partner)
                rc(src, src, s1s.at[c, 0], s1r.at[c, 0], (g, partner)).wait_recv()
            else:
                src = gblock(c, zfrom(k) * 2 + core)
                rc(src, src, s1s.at[c, k], s1r.at[c, k], (g, zpeer(k))).wait_recv()
                start(rc(src, src, f1s.at[c, k], f1r.at[c, k], (g, partner)))
        for k in range(1, Z):
            src = gblock(c, zfrom(k) * 2 + 1 - core)
            rc(src, src, f1s.at[c, k], f1r.at[c, k], (g, partner)).wait_recv()
        for d in eorder:
            oh = OH[pl.ds(pl.multiple_of(d * cap + core * R2, R2), R2), :]
            XS[c, d] = jnp.dot(oh, G[c], preferred_element_type=jnp.float32).astype(jnp.bfloat16)
            start(rc(XS.at[c, d], X.at[c, d, pl.ds(half, R2), :], x2s.at[c, d], x2r.at[c, d],
                     (epeer(d), j)))
        X[c, 0] = jnp.dot(OH[0:cap, :], G[c], preferred_element_type=jnp.float32).astype(jnp.bfloat16)

    def hblock(d, t):
        return H.at[d, :, pl.ds(pl.multiple_of(t * 128, 128), 128)]

    def gate_up(d):
        acc = jnp.dot(X[0, d], WC[0:W, :], preferred_element_type=jnp.float32)
        for c in range(1, CHUNKS):
            acc += jnp.dot(X[c, d], WC[c * W:(c + 1) * W, :], preferred_element_type=jnp.float32)
        gs = acc[:, :2 * hs]
        us = acc[:, 2 * hs:]
        hid = gs / (1.0 + jnp.exp(-gs)) * us
        hid = jnp.concatenate([hid[:R2], hid[R2:]], axis=1).astype(jnp.bfloat16)
        H[d, :, pl.ds(pl.multiple_of(j * 128, 128), 128)] = hid
        for k in zorder:
            start(rc(hblock(d, j), hblock(d, j), h3s.at[d, k], h3r.at[d, k], (g, zpeer(k))))
        start(rc(hblock(d, j), hblock(d, j), h3s.at[d, 0], h3r.at[d, 0], (g, partner)))

    gate_up(0)
    earrive = list(range(1, ep_size))
    for c in range(CHUNKS):
        for d in earrive:
            land = X.at[c, d, pl.ds(half, R2), :]
            rc(land, land, x2s.at[c, d], x2r.at[c, d], (epeer(d), j)).wait_recv()
            start(rc(land, land, xfs.at[c, d], xfr.at[c, d], (g, partner)))
    for k in range(1, tp_size):
        src = (j + tp_size - k) % tp_size
        rc(WDR.at[src], WDR.at[src], wds.at[k], wdr.at[k], (g, src)).wait_recv()
    for t in range(tp_size):
        for q in range(4):
            BW[t * 128 + q * hs:t * 128 + (q + 1) * hs, q * cols:(q + 1) * cols] = WDR[t, q % 2]
    for d in earrive:
        for c in range(CHUNKS):
            land = X.at[c, d, pl.ds(other, R2), :]
            rc(land, land, xfs.at[c, d], xfr.at[c, d], (g, partner)).wait_recv()
        gate_up(d)

    dorder = [0] + earrive
    for d in dorder:
        for k in [0] + list(range(1, Z)):
            if k == 0:
                src = hblock(d, partner)
                rc(src, src, h3s.at[d, 0], h3r.at[d, 0], (g, partner)).wait_recv()
            else:
                src = hblock(d, zfrom(k) * 2 + core)
                rc(src, src, h3s.at[d, k], h3r.at[d, k], (g, zpeer(k))).wait_recv()
                start(rc(src, src, hfs.at[d, k], hfr.at[d, k], (g, partner)))
    for d in earrive + [0]:
        for k in range(1, Z):
            src = hblock(d, zfrom(k) * 2 + 1 - core)
            rc(src, src, hfs.at[d, k], hfr.at[d, k], (g, partner)).wait_recv()
        res = jnp.dot(H[d], BW[...], preferred_element_type=jnp.float32).astype(jnp.bfloat16)
        if d == 0:
            RET[0, 0:R2, :] = res[:, :2 * cols]
            RET[0, R2:, :] = res[:, 2 * cols:]
        else:
            RS[d, 0:R2, :] = res[:, :2 * cols]
            RS[d, R2:, :] = res[:, 2 * cols:]
            start(rc(RS.at[d], RET.at[d], r4s.at[d], r4r.at[d], (epeer(d), j)))

    first = lax.rem(routing[:, 0:1], jnp.int32(local)) == 0
    s0 = jnp.where(first, share[:, 0:1], share[:, 1:2])
    s1 = jnp.where(first, share[:, 1:2], share[:, 0:1])
    total = jnp.dot(OHT[:, 0:cap], RET[0], preferred_element_type=jnp.float32)
    for d in earrive:
        rc(RS.at[d], RET.at[d], r4s.at[d], r4r.at[d], (epeer(d), j)).wait_recv()
        total += jnp.dot(OHT[:, d * cap:(d + 1) * cap], RET[d], preferred_element_type=jnp.float32)
    out[...] = (s0 * total[:, :cols] + s1 * total[:, cols:]).astype(out.dtype)
    for cp in sends:
        cp.wait_send()


def fused_body(ep_size, tp_size, tokens, norm_gain, routing, gate_share, w_gate, w_up, w_down):
    rows, D = tokens.shape
    local, _, hs = w_gate.shape
    n = routing.shape[0]
    cap = n * 4 // (local * ep_size)
    cols = D // tp_size
    W = D // CHUNKS
    Z = tp_size // 2
    R2 = cap // 2
    bf = jnp.bfloat16
    dma = pltpu.SemaphoreType.DMA
    vm = pltpu.VMEM
    return pl.pallas_call(
        functools.partial(kernel, ep_size, tp_size, cap),
        out_shape=jax.ShapeDtypeStruct((n, cols), bf),
        in_specs=[pl.BlockSpec(memory_space=pltpu.VMEM)] * 7,
        out_specs=pl.BlockSpec(memory_space=pltpu.VMEM),
        scratch_shapes=[
            vm((CHUNKS, n, W), bf),
            vm((ep_size * cap, n), bf),
            vm((n, ep_size * cap), bf),
            vm((CHUNKS, ep_size, R2, W), bf),
            vm((CHUNKS, ep_size, cap, W), bf),
            vm((ep_size, R2, tp_size * 128), bf),
            vm((ep_size, cap, 2 * cols), bf),
            vm((ep_size, cap, 2 * cols), bf),
            vm((D, 4 * hs), bf),
            vm((tp_size, local, hs, cols), bf),
            vm((tp_size * 4 * hs, 4 * cols), bf),
            dma((CHUNKS, Z)), dma((CHUNKS, Z)), dma((CHUNKS, Z)), dma((CHUNKS, Z)),
            dma((tp_size,)), dma((tp_size,)),
            dma((CHUNKS, ep_size)), dma((CHUNKS, ep_size)),
            dma((CHUNKS, ep_size)), dma((CHUNKS, ep_size)),
            dma((ep_size, Z)), dma((ep_size, Z)), dma((ep_size, Z)), dma((ep_size, Z)),
            dma((ep_size,)), dma((ep_size,)),
        ],
        compiler_params=pltpu.CompilerParams(collective_id=0, has_side_effects=True),
    )(tokens, norm_gain.reshape(1, D), routing, gate_share, w_gate, w_up, w_down)


def norm_rows(tokens, norm_gain):
    as_float = tokens.astype(jnp.float32)
    scaled = as_float * lax.rsqrt(jnp.mean(as_float * as_float, axis=-1, keepdims=True) + epsilon)
    return (scaled * norm_gain.astype(jnp.float32)).astype(jnp.bfloat16)


def fill_buffer(group, flat_target, slots, model_width):
    buffer = jnp.zeros((slots, model_width), jnp.bfloat16)
    return buffer.at[flat_target].set(jnp.repeat(group, 2, axis=0))


def body(tokens, norm_gain, routing, gate_share, w_gate, w_up, w_down):
    ep_size = lax.axis_size("ep")
    tp_size = lax.axis_size("tp")
    local_experts = w_gate.shape[0]
    experts = local_experts * ep_size
    group_rows = routing.shape[0]
    capacity = group_rows * 4 // experts
    model_width = tokens.shape[1]
    columns = model_width // tp_size
    normed = norm_rows(tokens, norm_gain)
    onehot = (routing[:, :, None] == jnp.arange(experts, dtype=jnp.int32)[None, None, :]).astype(
        jnp.int32
    )
    flat_hot = onehot.reshape(group_rows * 2, experts)
    ranking = jnp.cumsum(flat_hot, axis=0) - 1
    slot_pos = jnp.sum(ranking * flat_hot, axis=1).reshape(group_rows, 2)
    target = (routing * capacity + slot_pos).astype(jnp.int32)
    flat_target = target.reshape(-1)
    slice_len = capacity // tp_size
    tp_index = lax.axis_index("tp")
    group = lax.all_gather(normed, "tp", axis=0, tiled=True)
    buffer = fill_buffer(group, flat_target, experts * capacity, model_width)
    shaped = buffer.reshape(ep_size, local_experts, capacity, model_width)
    mine = lax.dynamic_slice_in_dim(shaped, tp_index * slice_len, slice_len, 2)
    mine = mine.reshape(ep_size, local_experts * slice_len, model_width)
    landed = lax.all_to_all(mine, "ep", split_axis=0, concat_axis=0, tiled=True)
    landed = landed.reshape(ep_size, local_experts, slice_len, model_width).transpose(1, 0, 2, 3)
    landed = landed.reshape(local_experts, ep_size * slice_len, model_width)
    full_gate, full_up, full_down = (
        lax.all_gather(w_gate, "tp", axis=2, tiled=True),
        lax.all_gather(w_up, "tp", axis=2, tiled=True),
        lax.all_gather(w_down, "tp", axis=1, tiled=True),
    )
    gate_sum = jnp.einsum("erd,edh->erh", landed, full_gate, preferred_element_type=jnp.float32)
    up_sum = jnp.einsum("erd,edh->erh", landed, full_up, preferred_element_type=jnp.float32)
    hidden = (jax.nn.silu(gate_sum) * up_sum).astype(jnp.bfloat16)
    produced = jnp.einsum(
        "erh,ehd->erd", hidden, full_down, preferred_element_type=jnp.float32
    ).astype(jnp.bfloat16)
    produced = produced.reshape(local_experts, ep_size, slice_len, model_width)
    blocks = lax.all_to_all(produced, "tp", split_axis=3, concat_axis=2, tiled=True)
    leaving = blocks.transpose(1, 0, 2, 3).reshape(ep_size, local_experts * capacity, columns)
    returned = lax.all_to_all(leaving, "ep", split_axis=0, concat_axis=0, tiled=True).reshape(
        experts * capacity, columns
    )
    picked_out = returned[target]
    mixed_out = jnp.sum(gate_share[:, :, None] * picked_out.astype(jnp.float32), axis=1)
    return mixed_out.astype(jnp.bfloat16)


def solution(mesh):
    ep_size, tp_size = mesh.shape["ep"], mesh.shape["tp"]

    def either(*arrays):
        local, _, hs = arrays[4].shape
        if ep_size == 4 and local == 2 and tp_size % 2 == 0 and 4 * hs == 128:
            return fused_body(ep_size, tp_size, *arrays)
        return body(*arrays)

    return jax.shard_map(
        either,
        mesh=mesh,
        in_specs=(
            P(("ep", "tp"), None),
            P(),
            P("ep", None),
            P("ep", None),
            P("ep", None, "tp"),
            P("ep", None, "tp"),
            P("ep", "tp", None),
        ),
        out_specs=P("ep", "tp"),
        check_vma=False,
    )
```

```python
import functools

import jax
import jax.numpy as jnp
from jax import lax
from jax.experimental import pallas as pl
from jax.experimental.pallas import tpu as pltpu
from jax.sharding import PartitionSpec as P

epsilon = 1e-06
MESH = pl.DeviceIdType.MESH
CHUNKS = 4


def kernel(ep_size, tp_size, cap, tok_h, gain_h, routing_h, share_h, wg, wu, wd_h, out,
           tok, gain, routing, share, wd, ins, SHS, SHR, shs, shr, G, OH, OHT, XS, X, H, RS, RET, WC, WDR, BW,
           s1s, s1r, f1s, f1r, wds, wdr, x2s, x2r, xfs, xfr,
           h3s, h3r, hfs, hfr, r4s, r4r):
    g = lax.axis_index("ep")
    j = lax.axis_index("tp")
    Z = tp_size // 2
    z = j // 2
    core = j % 2
    partner = z * 2 + (1 - core)
    rows, D = tok_h.shape
    W = D // CHUNKS
    R2 = cap // 2
    hs = wg.shape[1]
    side = ep_size // 2

    def zpeer(k):
        return ((z + k) % Z) * 2 + core

    def zfrom(k):
        return (z + Z - k) % Z

    def epeer(d):
        return ((g // side + d // side) % side) * side + (g % side + d % side) % side

    def rc(src, dst, ss, rs, dev):
        return pltpu.make_async_remote_copy(src_ref=src, dst_ref=dst, send_sem=ss,
                                            recv_sem=rs, device_id=dev, device_id_type=MESH)

    sends = []

    def start(cp):
        cp.start()
        sends.append(cp)

    bar = pltpu.get_barrier_semaphore()
    for k in range(1, tp_size):
        pl.semaphore_signal(bar, inc=1, device_id=(g, (j + k) % tp_size), device_id_type=MESH)
    for d in range(1, ep_size):
        pl.semaphore_signal(bar, inc=1, device_id=(epeer(d), j), device_id_type=MESH)

    def fetch(src, dst, i):
        cp = pltpu.make_async_copy(src, dst, ins.at[i])
        cp.start()
        return cp

    rows_in = [fetch(tok_h, tok, 0), fetch(gain_h, gain, 1)]
    ids_in = [fetch(routing_h, routing, 2), fetch(share_h, share, 3)]
    down_in = fetch(wd_h, wd, 4)
    weights_in = []
    for e in range(2):
        weights_in.append(fetch(wg.at[e], WC.at[pl.ds(e * hs, hs), :], 5 + e))
        weights_in.append(fetch(wu.at[e], WC.at[pl.ds((2 + e) * hs, hs), :], 7 + e))
    for cp in rows_in:
        cp.wait()
    x = tok[...].astype(jnp.float32)
    normed = x * lax.rsqrt(jnp.mean(x * x, axis=-1, keepdims=True) + epsilon)
    normed = (normed * gain[...]).astype(jnp.bfloat16)

    def gblock(c, t):
        return G.at[c, pl.ds(pl.multiple_of(t * rows, rows), rows), :]

    for c in range(CHUNKS):
        G[c, pl.ds(pl.multiple_of(j * rows, rows), rows), :] = normed[:, c * W:(c + 1) * W]

    pl.semaphore_wait(bar, tp_size - 1 + ep_size - 1)

    zorder = [Z // 2] + [k for k in range(1, Z) if k != Z // 2]
    for c in range(CHUNKS):
        for k in zorder:
            start(rc(gblock(c, j), gblock(c, j), s1s.at[c, k], s1r.at[c, k], (g, zpeer(k))))
        start(rc(gblock(c, j), gblock(c, j), s1s.at[c, 0], s1r.at[c, 0], (g, partner)))
    cols = D // tp_size
    for cp in ids_in:
        cp.wait()

    n = routing.shape[1]
    local = wg.shape[0]
    rel_row = jnp.bitwise_xor(lax.div(routing[0:1, :], jnp.int32(local)), g)
    first = lax.rem(routing[0:1, :], jnp.int32(local)) == 0
    s0_row = jnp.where(first, share[0:1, :], share[1:2, :])
    s1_row = jnp.where(first, share[1:2, :], share[0:1, :])
    packed = jnp.concatenate([rel_row.astype(jnp.float32), s0_row, s1_row,
                              jnp.zeros((125, n), jnp.float32)], axis=0)
    columns = jnp.transpose(packed)
    rel = columns[:, 0:1].astype(jnp.int32)
    s0 = columns[:, 1:2]
    s1 = columns[:, 2:3]
    hot = (lax.broadcasted_iota(jnp.int32, (n, 128), 1) == rel)
    low = lax.broadcasted_iota(jnp.int32, (n, n), 1) < lax.broadcasted_iota(jnp.int32, (n, n), 0)
    rank = jnp.dot(low.astype(jnp.bfloat16), hot.astype(jnp.bfloat16),
                   preferred_element_type=jnp.float32)
    pos = jnp.sum(jnp.where(hot, rank, 0.0), axis=1, keepdims=True)
    slot = rel.astype(jnp.float32) * cap + pos
    slots = ep_size * cap
    mine = lax.broadcasted_iota(jnp.int32, (n, slots), 1).astype(jnp.float32) == slot
    OHT[...] = mine.astype(jnp.bfloat16)
    both = jnp.concatenate([jnp.sum(jnp.where(mine, s0, 0.0), axis=0, keepdims=True),
                            jnp.sum(jnp.where(mine, s1, 0.0), axis=0, keepdims=True),
                            jnp.zeros((6, slots), jnp.float32)], axis=0)
    SHR[0] = both[:, 0:cap]
    for d in range(1, ep_size):
        SHS[d] = both[:, d * cap:(d + 1) * cap]
        start(rc(SHS.at[d], SHR.at[d], shs.at[d], shr.at[d], (epeer(d), j)))
    slot_row = jnp.transpose(jnp.broadcast_to(slot, (n, 128)))[0:1, :]
    OH[...] = (lax.broadcasted_iota(jnp.int32, (slots, n), 0).astype(jnp.float32)
               == slot_row).astype(jnp.bfloat16)
    for cp in weights_in + [down_in]:
        cp.wait()
    BW[...] = jnp.zeros_like(BW)

    half = pl.multiple_of(core * R2, R2)
    other = pl.multiple_of((1 - core) * R2, R2)
    eorder = [ep_size - 1] + list(range(1, ep_size - 1))

    for c in range(CHUNKS):
        for k in [0] + list(range(1, Z)):
            if k == 0:
                src = gblock(c, partner)
                rc(src, src, s1s.at[c, 0], s1r.at[c, 0], (g, partner)).wait_recv()
            else:
                src = gblock(c, zfrom(k) * 2 + core)
                rc(src, src, s1s.at[c, k], s1r.at[c, k], (g, zpeer(k))).wait_recv()
                start(rc(src, src, f1s.at[c, k], f1r.at[c, k], (g, partner)))
        for k in range(1, Z):
            src = gblock(c, zfrom(k) * 2 + 1 - core)
            rc(src, src, f1s.at[c, k], f1r.at[c, k], (g, partner)).wait_recv()
        for d in eorder:
            oh = OH[pl.ds(pl.multiple_of(d * cap + core * R2, R2), R2), :]
            XS[c, d] = jnp.dot(oh, G[c], preferred_element_type=jnp.float32).astype(jnp.bfloat16)
            start(rc(XS.at[c, d], X.at[c, d, pl.ds(half, R2), :], x2s.at[c, d], x2r.at[c, d],
                     (epeer(d), j)))
        X[c, 0] = jnp.dot(OH[0:cap, :], G[c], preferred_element_type=jnp.float32).astype(jnp.bfloat16)

    for k in range(1, tp_size):
        dst = (j + k) % tp_size
        start(rc(wd.at[:, :, pl.ds(pl.multiple_of(dst * cols, cols), cols)], WDR.at[j],
                 wds.at[k], wdr.at[k], (g, dst)))
    WDR[j] = wd[:, :, pl.ds(pl.multiple_of(j * cols, cols), cols)]

    def hblock(d, t):
        return H.at[d, :, pl.ds(pl.multiple_of(t * 128, 128), 128)]

    def gate_up(d):
        acc = None
        for c in range(CHUNKS):
            part = lax.dot_general(X[c, d], WC[:, c * W:(c + 1) * W], (((1,), (1,)), ((), ())),
                                   preferred_element_type=jnp.float32)
            acc = part if acc is None else acc + part
        gs = acc[:, :2 * hs]
        us = acc[:, 2 * hs:]
        hid = gs / (1.0 + jnp.exp(-gs)) * us
        hid = jnp.concatenate([hid[:R2], hid[R2:]], axis=1).astype(jnp.bfloat16)
        H[d, :, pl.ds(pl.multiple_of(j * 128, 128), 128)] = hid
        for k in zorder:
            start(rc(hblock(d, j), hblock(d, j), h3s.at[d, k], h3r.at[d, k], (g, zpeer(k))))
        start(rc(hblock(d, j), hblock(d, j), h3s.at[d, 0], h3r.at[d, 0], (g, partner)))

    def take_hidden(d):
        for k in [0] + list(range(1, Z)):
            if k == 0:
                src = hblock(d, partner)
                rc(src, src, h3s.at[d, 0], h3r.at[d, 0], (g, partner)).wait_recv()
            else:
                src = hblock(d, zfrom(k) * 2 + core)
                rc(src, src, h3s.at[d, k], h3r.at[d, k], (g, zpeer(k))).wait_recv()
                start(rc(src, src, hfs.at[d, k], hfr.at[d, k], (g, partner)))

    gate_up(0)
    earrive = list(range(1, ep_size))
    for c in range(CHUNKS):
        for d in earrive:
            land = X.at[c, d, pl.ds(half, R2), :]
            rc(land, land, x2s.at[c, d], x2r.at[c, d], (epeer(d), j)).wait_recv()
            start(rc(land, land, xfs.at[c, d], xfr.at[c, d], (g, partner)))
    take_hidden(0)
    for k in range(1, tp_size):
        src = (j + tp_size - k) % tp_size
        rc(WDR.at[src], WDR.at[src], wds.at[k], wdr.at[k], (g, src)).wait_recv()
    for t in range(tp_size):
        for q in range(4):
            BW[t * 128 + q * hs:t * 128 + (q + 1) * hs, q * cols:(q + 1) * cols] = WDR[t, q % 2]
    for d in earrive:
        for c in range(CHUNKS):
            land = X.at[c, d, pl.ds(other, R2), :]
            rc(land, land, xfs.at[c, d], xfr.at[c, d], (g, partner)).wait_recv()
        gate_up(d)

    def down(d):
        for k in range(1, Z):
            src = hblock(d, zfrom(k) * 2 + 1 - core)
            rc(src, src, hfs.at[d, k], hfr.at[d, k], (g, partner)).wait_recv()
        res = jnp.dot(H[d], BW[...], preferred_element_type=jnp.float32)
        res = res.astype(jnp.bfloat16).astype(jnp.float32)
        a = shares[:, 8 * d:8 * d + 1]
        b = shares[:, 8 * d + 1:8 * d + 2]
        target = RET if d == 0 else RS
        target[d, 0:R2, :] = (a[:R2] * res[:, :cols]
                              + b[:R2] * res[:, cols:2 * cols]).astype(jnp.bfloat16)
        target[d, R2:, :] = (a[R2:] * res[:, 2 * cols:3 * cols]
                             + b[R2:] * res[:, 3 * cols:]).astype(jnp.bfloat16)
        if d:
            start(rc(RS.at[d], RET.at[d], r4s.at[d], r4r.at[d], (epeer(d), j)))

    for d in earrive:
        rc(SHS.at[d], SHR.at[d], shs.at[d], shr.at[d], (epeer(d), j)).wait_recv()
    shares = jnp.transpose(jnp.concatenate(
        [SHR[d] for d in range(ep_size)] + [jnp.zeros((128 - 8 * ep_size, cap), jnp.float32)], axis=0))
    down(0)
    take_hidden(1)
    for d in earrive[1:]:
        take_hidden(d)
        down(d - 1)
    down(ep_size - 1)

    total = jnp.dot(OHT[:, 0:cap], RET[0], preferred_element_type=jnp.float32)
    for d in earrive:
        rc(RS.at[d], RET.at[d], r4s.at[d], r4r.at[d], (epeer(d), j)).wait_recv()
        total += jnp.dot(OHT[:, d * cap:(d + 1) * cap], RET[d], preferred_element_type=jnp.float32)
    out[...] = total.astype(out.dtype)
    for cp in sends:
        cp.wait_send()


def fused_body(ep_size, tp_size, tokens, norm_gain, routing, gate_share, w_gate, w_up, w_down):
    rows, D = tokens.shape
    local, _, hs = w_gate.shape
    n = routing.shape[0]
    cap = n * 4 // (local * ep_size)
    cols = D // tp_size
    W = D // CHUNKS
    Z = tp_size // 2
    R2 = cap // 2
    bf = jnp.bfloat16
    dma = pltpu.SemaphoreType.DMA
    vm = pltpu.VMEM
    return pl.pallas_call(
        functools.partial(kernel, ep_size, tp_size, cap),
        out_shape=jax.ShapeDtypeStruct((n, cols), bf),
        in_specs=[pl.BlockSpec(memory_space=pltpu.HBM)] * 7,
        out_specs=pl.BlockSpec(memory_space=pltpu.VMEM),
        scratch_shapes=[
            vm((rows, D), bf), vm((1, D), jnp.float32),
            vm((2, n), jnp.int32), vm((2, n), jnp.float32), vm((local, hs, D), bf),
            dma((9,)),
            vm((ep_size, 8, cap), jnp.float32), vm((ep_size, 8, cap), jnp.float32),
            dma((ep_size,)), dma((ep_size,)),
            vm((CHUNKS, n, W), bf),
            vm((ep_size * cap, n), bf),
            vm((n, ep_size * cap), bf),
            vm((CHUNKS, ep_size, R2, W), bf),
            vm((CHUNKS, ep_size, cap, W), bf),
            vm((ep_size, R2, tp_size * 128), bf),
            vm((ep_size, cap, cols), bf),
            vm((ep_size, cap, cols), bf),
            vm((4 * hs, D), bf),
            vm((tp_size, local, hs, cols), bf),
            vm((tp_size * 4 * hs, 4 * cols), bf),
            dma((CHUNKS, Z)), dma((CHUNKS, Z)), dma((CHUNKS, Z)), dma((CHUNKS, Z)),
            dma((tp_size,)), dma((tp_size,)),
            dma((CHUNKS, ep_size)), dma((CHUNKS, ep_size)),
            dma((CHUNKS, ep_size)), dma((CHUNKS, ep_size)),
            dma((ep_size, Z)), dma((ep_size, Z)), dma((ep_size, Z)), dma((ep_size, Z)),
            dma((ep_size,)), dma((ep_size,)),
        ],
        compiler_params=pltpu.CompilerParams(collective_id=0, has_side_effects=True,
                                             vmem_limit_bytes=67043328),
    )(tokens, norm_gain.reshape(1, D), routing.T, gate_share.T, w_gate.swapaxes(1, 2),
      w_up.swapaxes(1, 2), w_down)


def norm_rows(tokens, norm_gain):
    as_float = tokens.astype(jnp.float32)
    scaled = as_float * lax.rsqrt(jnp.mean(as_float * as_float, axis=-1, keepdims=True) + epsilon)
    return (scaled * norm_gain.astype(jnp.float32)).astype(jnp.bfloat16)


def fill_buffer(group, flat_target, slots, model_width):
    buffer = jnp.zeros((slots, model_width), jnp.bfloat16)
    return buffer.at[flat_target].set(jnp.repeat(group, 2, axis=0))


def body(tokens, norm_gain, routing, gate_share, w_gate, w_up, w_down):
    ep_size = lax.axis_size("ep")
    tp_size = lax.axis_size("tp")
    local_experts = w_gate.shape[0]
    experts = local_experts * ep_size
    group_rows = routing.shape[0]
    capacity = group_rows * 4 // experts
    model_width = tokens.shape[1]
    columns = model_width // tp_size
    normed = norm_rows(tokens, norm_gain)
    onehot = (routing[:, :, None] == jnp.arange(experts, dtype=jnp.int32)[None, None, :]).astype(
        jnp.int32
    )
    flat_hot = onehot.reshape(group_rows * 2, experts)
    ranking = jnp.cumsum(flat_hot, axis=0) - 1
    slot_pos = jnp.sum(ranking * flat_hot, axis=1).reshape(group_rows, 2)
    target = (routing * capacity + slot_pos).astype(jnp.int32)
    flat_target = target.reshape(-1)
    slice_len = capacity // tp_size
    tp_index = lax.axis_index("tp")
    group = lax.all_gather(normed, "tp", axis=0, tiled=True)
    buffer = fill_buffer(group, flat_target, experts * capacity, model_width)
    shaped = buffer.reshape(ep_size, local_experts, capacity, model_width)
    mine = lax.dynamic_slice_in_dim(shaped, tp_index * slice_len, slice_len, 2)
    mine = mine.reshape(ep_size, local_experts * slice_len, model_width)
    landed = lax.all_to_all(mine, "ep", split_axis=0, concat_axis=0, tiled=True)
    landed = landed.reshape(ep_size, local_experts, slice_len, model_width).transpose(1, 0, 2, 3)
    landed = landed.reshape(local_experts, ep_size * slice_len, model_width)
    full_gate, full_up, full_down = (
        lax.all_gather(w_gate, "tp", axis=2, tiled=True),
        lax.all_gather(w_up, "tp", axis=2, tiled=True),
        lax.all_gather(w_down, "tp", axis=1, tiled=True),
    )
    gate_sum = jnp.einsum("erd,edh->erh", landed, full_gate, preferred_element_type=jnp.float32)
    up_sum = jnp.einsum("erd,edh->erh", landed, full_up, preferred_element_type=jnp.float32)
    hidden = (jax.nn.silu(gate_sum) * up_sum).astype(jnp.bfloat16)
    produced = jnp.einsum(
        "erh,ehd->erd", hidden, full_down, preferred_element_type=jnp.float32
    ).astype(jnp.bfloat16)
    produced = produced.reshape(local_experts, ep_size, slice_len, model_width)
    blocks = lax.all_to_all(produced, "tp", split_axis=3, concat_axis=2, tiled=True)
    leaving = blocks.transpose(1, 0, 2, 3).reshape(ep_size, local_experts * capacity, columns)
    returned = lax.all_to_all(leaving, "ep", split_axis=0, concat_axis=0, tiled=True).reshape(
        experts * capacity, columns
    )
    picked_out = returned[target]
    mixed_out = jnp.sum(gate_share[:, :, None] * picked_out.astype(jnp.float32), axis=1)
    return mixed_out.astype(jnp.bfloat16)


def solution(mesh):
    ep_size, tp_size = mesh.shape["ep"], mesh.shape["tp"]

    def either(*arrays):
        local, _, hs = arrays[4].shape
        if ep_size == 4 and local == 2 and tp_size % 2 == 0 and 4 * hs == 128:
            return fused_body(ep_size, tp_size, *arrays)
        return body(*arrays)

    return jax.shard_map(
        either,
        mesh=mesh,
        in_specs=(
            P(("ep", "tp"), None),
            P(),
            P("ep", None),
            P("ep", None),
            P("ep", None, "tp"),
            P("ep", None, "tp"),
            P("ep", "tp", None),
        ),
        out_specs=P("ep", "tp"),
        check_vma=False,
    )
```

```python
import functools

import jax
import jax.numpy as jnp
from jax import lax
from jax.experimental import pallas as pl
from jax.experimental.pallas import tpu as pltpu
from jax.sharding import PartitionSpec as P

epsilon = 1e-06
MESH = pl.DeviceIdType.MESH
CHUNKS = 2


def kernel(ep_size, tp_size, cap, tok_h, gain_h, routing_h, share_h, wg, wu, wd_h, out,
           tok, gain, routing, share, wd, ins, SHS, SHR, shs, shr, G, OH, OHT, XS, X, H, RS, RET, WC, WDR, BW,
           s1s, s1r, f1s, f1r, wds, wdr, x2s, x2r, xfs, xfr,
           h3s, h3r, hfs, hfr, r4s, r4r):
    g = lax.axis_index("ep")
    j = lax.axis_index("tp")
    Z = tp_size // 2
    z = j // 2
    core = j % 2
    partner = z * 2 + (1 - core)
    rows, D = tok_h.shape
    W = D // CHUNKS
    R2 = cap // 2
    hs = wg.shape[1]
    side = ep_size // 2

    def zpeer(k):
        return ((z + k) % Z) * 2 + core

    def zfrom(k):
        return (z + Z - k) % Z

    def epeer(d):
        return ((g // side + d // side) % side) * side + (g % side + d % side) % side

    def rc(src, dst, ss, rs, dev):
        return pltpu.make_async_remote_copy(src_ref=src, dst_ref=dst, send_sem=ss,
                                            recv_sem=rs, device_id=dev, device_id_type=MESH)

    sends = []

    def start(cp):
        cp.start()
        sends.append(cp)

    bar = pltpu.get_barrier_semaphore()
    for k in range(1, tp_size):
        pl.semaphore_signal(bar, inc=1, device_id=(g, (j + k) % tp_size), device_id_type=MESH)
    for d in range(1, ep_size):
        pl.semaphore_signal(bar, inc=1, device_id=(epeer(d), j), device_id_type=MESH)

    def fetch(src, dst, i):
        cp = pltpu.make_async_copy(src, dst, ins.at[i])
        cp.start()
        return cp

    rows_in = [fetch(tok_h, tok, 0), fetch(gain_h, gain, 1)]
    ids_in = [fetch(routing_h, routing, 2), fetch(share_h, share, 3)]
    down_in = fetch(wd_h, wd, 4)
    weights_in = []
    for e in range(2):
        weights_in.append(fetch(wg.at[e], WC.at[pl.ds(e * hs, hs), :], 5 + e))
        weights_in.append(fetch(wu.at[e], WC.at[pl.ds((2 + e) * hs, hs), :], 7 + e))
    for cp in rows_in:
        cp.wait()
    x = tok[...].astype(jnp.float32)
    normed = x * lax.rsqrt(jnp.mean(x * x, axis=-1, keepdims=True) + epsilon)
    normed = (normed * gain[...]).astype(jnp.bfloat16)

    def gblock(c, t):
        return G.at[c, pl.ds(pl.multiple_of(t * rows, rows), rows), :]

    for c in range(CHUNKS):
        G[c, pl.ds(pl.multiple_of(j * rows, rows), rows), :] = normed[:, c * W:(c + 1) * W]

    pl.semaphore_wait(bar, tp_size - 1 + ep_size - 1)

    zorder = [k for k in range(1, Z) if k != Z // 2] + [Z // 2]
    for c in range(CHUNKS):
        for k in zorder:
            start(rc(gblock(c, j), gblock(c, j), s1s.at[c, k], s1r.at[c, k], (g, zpeer(k))))
        start(rc(gblock(c, j), gblock(c, j), s1s.at[c, 0], s1r.at[c, 0], (g, partner)))
    cols = D // tp_size
    for cp in ids_in:
        cp.wait()

    n = routing.shape[1]
    local = wg.shape[0]
    rel_row = jnp.bitwise_xor(lax.div(routing[0:1, :], jnp.int32(local)), g)
    first = lax.rem(routing[0:1, :], jnp.int32(local)) == 0
    s0_row = jnp.where(first, share[0:1, :], share[1:2, :])
    s1_row = jnp.where(first, share[1:2, :], share[0:1, :])
    packed = jnp.concatenate([rel_row.astype(jnp.float32), s0_row, s1_row,
                              jnp.zeros((125, n), jnp.float32)], axis=0)
    columns = jnp.transpose(packed)
    rel = columns[:, 0:1].astype(jnp.int32)
    s0 = columns[:, 1:2]
    s1 = columns[:, 2:3]
    hot = (lax.broadcasted_iota(jnp.int32, (n, 128), 1) == rel)
    low = lax.broadcasted_iota(jnp.int32, (n, n), 1) < lax.broadcasted_iota(jnp.int32, (n, n), 0)
    rank = jnp.dot(low.astype(jnp.bfloat16), hot.astype(jnp.bfloat16),
                   preferred_element_type=jnp.float32)
    pos = jnp.sum(jnp.where(hot, rank, 0.0), axis=1, keepdims=True)
    slot = rel.astype(jnp.float32) * cap + pos
    slots = ep_size * cap
    mine = lax.broadcasted_iota(jnp.int32, (n, slots), 1).astype(jnp.float32) == slot
    OHT[...] = mine.astype(jnp.bfloat16)
    both = jnp.concatenate([jnp.sum(jnp.where(mine, s0, 0.0), axis=0, keepdims=True),
                            jnp.sum(jnp.where(mine, s1, 0.0), axis=0, keepdims=True),
                            jnp.zeros((6, slots), jnp.float32)], axis=0)
    SHR[0] = both[:, 0:cap]
    for d in range(1, ep_size):
        SHS[d] = both[:, d * cap:(d + 1) * cap]
        start(rc(SHS.at[d], SHR.at[d], shs.at[d], shr.at[d], (epeer(d), j)))
    slot_row = jnp.transpose(jnp.broadcast_to(slot, (n, 128)))[0:1, :]
    OH[...] = (lax.broadcasted_iota(jnp.int32, (slots, n), 0).astype(jnp.float32)
               == slot_row).astype(jnp.bfloat16)
    for cp in weights_in + [down_in]:
        cp.wait()
    BW[...] = jnp.zeros_like(BW)

    half = pl.multiple_of(core * R2, R2)
    other = pl.multiple_of((1 - core) * R2, R2)
    eorder = [ep_size - 1] + list(range(1, ep_size - 1))

    for c in range(CHUNKS):
        for k in [0] + list(range(1, Z)):
            if k == 0:
                src = gblock(c, partner)
                rc(src, src, s1s.at[c, 0], s1r.at[c, 0], (g, partner)).wait_recv()
            else:
                src = gblock(c, zfrom(k) * 2 + core)
                rc(src, src, s1s.at[c, k], s1r.at[c, k], (g, zpeer(k))).wait_recv()
                start(rc(src, src, f1s.at[c, k], f1r.at[c, k], (g, partner)))
        for k in range(1, Z):
            src = gblock(c, zfrom(k) * 2 + 1 - core)
            rc(src, src, f1s.at[c, k], f1r.at[c, k], (g, partner)).wait_recv()
        for d in eorder:
            oh = OH[pl.ds(pl.multiple_of(d * cap + core * R2, R2), R2), :]
            XS[c, d] = jnp.dot(oh, G[c], preferred_element_type=jnp.float32).astype(jnp.bfloat16)
            start(rc(XS.at[c, d], X.at[c, d, pl.ds(half, R2), :], x2s.at[c, d], x2r.at[c, d],
                     (epeer(d), j)))
        X[c, 0] = jnp.dot(OH[0:cap, :], G[c], preferred_element_type=jnp.float32).astype(jnp.bfloat16)

    for k in range(1, tp_size):
        dst = (j + k) % tp_size
        start(rc(wd.at[:, :, pl.ds(pl.multiple_of(dst * cols, cols), cols)], WDR.at[j],
                 wds.at[k], wdr.at[k], (g, dst)))
    WDR[j] = wd[:, :, pl.ds(pl.multiple_of(j * cols, cols), cols)]

    def hblock(d, t):
        return H.at[d, :, pl.ds(pl.multiple_of(t * 128, 128), 128)]

    def gate_up(d):
        acc = None
        for c in range(CHUNKS):
            part = lax.dot_general(X[c, d], WC[:, c * W:(c + 1) * W], (((1,), (1,)), ((), ())),
                                   preferred_element_type=jnp.float32)
            acc = part if acc is None else acc + part
        gs = acc[:, :2 * hs]
        us = acc[:, 2 * hs:]
        hid = gs / (1.0 + jnp.exp(-gs)) * us
        hid = jnp.concatenate([hid[:R2], hid[R2:]], axis=1).astype(jnp.bfloat16)
        H[d, :, pl.ds(pl.multiple_of(j * 128, 128), 128)] = hid
        for k in zorder:
            start(rc(hblock(d, j), hblock(d, j), h3s.at[d, k], h3r.at[d, k], (g, zpeer(k))))
        start(rc(hblock(d, j), hblock(d, j), h3s.at[d, 0], h3r.at[d, 0], (g, partner)))

    def take_hidden(d):
        for k in [0] + list(range(1, Z)):
            if k == 0:
                src = hblock(d, partner)
                rc(src, src, h3s.at[d, 0], h3r.at[d, 0], (g, partner)).wait_recv()
            else:
                src = hblock(d, zfrom(k) * 2 + core)
                rc(src, src, h3s.at[d, k], h3r.at[d, k], (g, zpeer(k))).wait_recv()
                start(rc(src, src, hfs.at[d, k], hfr.at[d, k], (g, partner)))

    gate_up(0)
    earrive = list(range(1, ep_size))
    for c in range(CHUNKS):
        for d in earrive:
            land = X.at[c, d, pl.ds(half, R2), :]
            rc(land, land, x2s.at[c, d], x2r.at[c, d], (epeer(d), j)).wait_recv()
            start(rc(land, land, xfs.at[c, d], xfr.at[c, d], (g, partner)))
    take_hidden(0)
    for k in range(1, tp_size):
        src = (j + tp_size - k) % tp_size
        rc(WDR.at[src], WDR.at[src], wds.at[k], wdr.at[k], (g, src)).wait_recv()
    for t in range(tp_size):
        for q in range(4):
            BW[t * 128 + q * hs:t * 128 + (q + 1) * hs, q * cols:(q + 1) * cols] = WDR[t, q % 2]
    for d in earrive:
        for c in range(CHUNKS):
            land = X.at[c, d, pl.ds(other, R2), :]
            rc(land, land, xfs.at[c, d], xfr.at[c, d], (g, partner)).wait_recv()
        gate_up(d)

    def down(d):
        for k in range(1, Z):
            src = hblock(d, zfrom(k) * 2 + 1 - core)
            rc(src, src, hfs.at[d, k], hfr.at[d, k], (g, partner)).wait_recv()
        res = jnp.dot(H[d], BW[...], preferred_element_type=jnp.float32)
        res = res.astype(jnp.bfloat16).astype(jnp.float32)
        a = shares[:, 8 * d:8 * d + 1]
        b = shares[:, 8 * d + 1:8 * d + 2]
        target = RET if d == 0 else RS
        target[d, 0:R2, :] = (a[:R2] * res[:, :cols]
                              + b[:R2] * res[:, cols:2 * cols]).astype(jnp.bfloat16)
        target[d, R2:, :] = (a[R2:] * res[:, 2 * cols:3 * cols]
                             + b[R2:] * res[:, 3 * cols:]).astype(jnp.bfloat16)
        if d:
            start(rc(RS.at[d], RET.at[d], r4s.at[d], r4r.at[d], (epeer(d), j)))

    for d in earrive:
        rc(SHS.at[d], SHR.at[d], shs.at[d], shr.at[d], (epeer(d), j)).wait_recv()
    shares = jnp.transpose(jnp.concatenate(
        [SHR[d] for d in range(ep_size)] + [jnp.zeros((128 - 8 * ep_size, cap), jnp.float32)], axis=0))
    down(0)
    take_hidden(1)
    for d in earrive[1:]:
        take_hidden(d)
        down(d - 1)
    down(ep_size - 1)

    total = jnp.dot(OHT[:, 0:cap], RET[0], preferred_element_type=jnp.float32)
    for d in earrive:
        rc(RS.at[d], RET.at[d], r4s.at[d], r4r.at[d], (epeer(d), j)).wait_recv()
        total += jnp.dot(OHT[:, d * cap:(d + 1) * cap], RET[d], preferred_element_type=jnp.float32)
    out[...] = total.astype(out.dtype)
    for cp in sends:
        cp.wait_send()


def fused_body(ep_size, tp_size, tokens, norm_gain, routing, gate_share, w_gate, w_up, w_down):
    rows, D = tokens.shape
    local, _, hs = w_gate.shape
    n = routing.shape[0]
    cap = n * 4 // (local * ep_size)
    cols = D // tp_size
    W = D // CHUNKS
    Z = tp_size // 2
    R2 = cap // 2
    bf = jnp.bfloat16
    dma = pltpu.SemaphoreType.DMA
    vm = pltpu.VMEM
    return pl.pallas_call(
        functools.partial(kernel, ep_size, tp_size, cap),
        out_shape=jax.ShapeDtypeStruct((n, cols), bf),
        in_specs=[pl.BlockSpec(memory_space=pltpu.HBM)] * 7,
        out_specs=pl.BlockSpec(memory_space=pltpu.VMEM),
        scratch_shapes=[
            vm((rows, D), bf), vm((1, D), jnp.float32),
            vm((2, n), jnp.int32), vm((2, n), jnp.float32), vm((local, hs, D), bf),
            dma((9,)),
            vm((ep_size, 8, cap), jnp.float32), vm((ep_size, 8, cap), jnp.float32),
            dma((ep_size,)), dma((ep_size,)),
            vm((CHUNKS, n, W), bf),
            vm((ep_size * cap, n), bf),
            vm((n, ep_size * cap), bf),
            vm((CHUNKS, ep_size, R2, W), bf),
            vm((CHUNKS, ep_size, cap, W), bf),
            vm((ep_size, R2, tp_size * 128), bf),
            vm((ep_size, cap, cols), bf),
            vm((ep_size, cap, cols), bf),
            vm((4 * hs, D), bf),
            vm((tp_size, local, hs, cols), bf),
            vm((tp_size * 4 * hs, 4 * cols), bf),
            dma((CHUNKS, Z)), dma((CHUNKS, Z)), dma((CHUNKS, Z)), dma((CHUNKS, Z)),
            dma((tp_size,)), dma((tp_size,)),
            dma((CHUNKS, ep_size)), dma((CHUNKS, ep_size)),
            dma((CHUNKS, ep_size)), dma((CHUNKS, ep_size)),
            dma((ep_size, Z)), dma((ep_size, Z)), dma((ep_size, Z)), dma((ep_size, Z)),
            dma((ep_size,)), dma((ep_size,)),
        ],
        compiler_params=pltpu.CompilerParams(collective_id=0, has_side_effects=True,
                                             vmem_limit_bytes=67043328),
    )(tokens, norm_gain.reshape(1, D), routing.T, gate_share.T, w_gate.swapaxes(1, 2),
      w_up.swapaxes(1, 2), w_down)


def norm_rows(tokens, norm_gain):
    as_float = tokens.astype(jnp.float32)
    scaled = as_float * lax.rsqrt(jnp.mean(as_float * as_float, axis=-1, keepdims=True) + epsilon)
    return (scaled * norm_gain.astype(jnp.float32)).astype(jnp.bfloat16)


def fill_buffer(group, flat_target, slots, model_width):
    buffer = jnp.zeros((slots, model_width), jnp.bfloat16)
    return buffer.at[flat_target].set(jnp.repeat(group, 2, axis=0))


def body(tokens, norm_gain, routing, gate_share, w_gate, w_up, w_down):
    ep_size = lax.axis_size("ep")
    tp_size = lax.axis_size("tp")
    local_experts = w_gate.shape[0]
    experts = local_experts * ep_size
    group_rows = routing.shape[0]
    capacity = group_rows * 4 // experts
    model_width = tokens.shape[1]
    columns = model_width // tp_size
    normed = norm_rows(tokens, norm_gain)
    onehot = (routing[:, :, None] == jnp.arange(experts, dtype=jnp.int32)[None, None, :]).astype(
        jnp.int32
    )
    flat_hot = onehot.reshape(group_rows * 2, experts)
    ranking = jnp.cumsum(flat_hot, axis=0) - 1
    slot_pos = jnp.sum(ranking * flat_hot, axis=1).reshape(group_rows, 2)
    target = (routing * capacity + slot_pos).astype(jnp.int32)
    flat_target = target.reshape(-1)
    slice_len = capacity // tp_size
    tp_index = lax.axis_index("tp")
    group = lax.all_gather(normed, "tp", axis=0, tiled=True)
    buffer = fill_buffer(group, flat_target, experts * capacity, model_width)
    shaped = buffer.reshape(ep_size, local_experts, capacity, model_width)
    mine = lax.dynamic_slice_in_dim(shaped, tp_index * slice_len, slice_len, 2)
    mine = mine.reshape(ep_size, local_experts * slice_len, model_width)
    landed = lax.all_to_all(mine, "ep", split_axis=0, concat_axis=0, tiled=True)
    landed = landed.reshape(ep_size, local_experts, slice_len, model_width).transpose(1, 0, 2, 3)
    landed = landed.reshape(local_experts, ep_size * slice_len, model_width)
    full_gate, full_up, full_down = (
        lax.all_gather(w_gate, "tp", axis=2, tiled=True),
        lax.all_gather(w_up, "tp", axis=2, tiled=True),
        lax.all_gather(w_down, "tp", axis=1, tiled=True),
    )
    gate_sum = jnp.einsum("erd,edh->erh", landed, full_gate, preferred_element_type=jnp.float32)
    up_sum = jnp.einsum("erd,edh->erh", landed, full_up, preferred_element_type=jnp.float32)
    hidden = (jax.nn.silu(gate_sum) * up_sum).astype(jnp.bfloat16)
    produced = jnp.einsum(
        "erh,ehd->erd", hidden, full_down, preferred_element_type=jnp.float32
    ).astype(jnp.bfloat16)
    produced = produced.reshape(local_experts, ep_size, slice_len, model_width)
    blocks = lax.all_to_all(produced, "tp", split_axis=3, concat_axis=2, tiled=True)
    leaving = blocks.transpose(1, 0, 2, 3).reshape(ep_size, local_experts * capacity, columns)
    returned = lax.all_to_all(leaving, "ep", split_axis=0, concat_axis=0, tiled=True).reshape(
        experts * capacity, columns
    )
    picked_out = returned[target]
    mixed_out = jnp.sum(gate_share[:, :, None] * picked_out.astype(jnp.float32), axis=1)
    return mixed_out.astype(jnp.bfloat16)


def solution(mesh):
    ep_size, tp_size = mesh.shape["ep"], mesh.shape["tp"]

    def either(*arrays):
        local, _, hs = arrays[4].shape
        if ep_size == 4 and local == 2 and tp_size % 2 == 0 and 4 * hs == 128:
            return fused_body(ep_size, tp_size, *arrays)
        return body(*arrays)

    return jax.shard_map(
        either,
        mesh=mesh,
        in_specs=(
            P(("ep", "tp"), None),
            P(),
            P("ep", None),
            P("ep", None),
            P("ep", None, "tp"),
            P("ep", None, "tp"),
            P("ep", "tp", None),
        ),
        out_specs=P("ep", "tp"),
        check_vma=False,
    )
```
